32 devices in a mesh: sp: 8 (over z, x), tp: 4 (over y, core).
Axes of the slice: x: 2, y: 2, z: 4, core: 2. Of those that a mesh axis runs over, the one named last changes fastest.
Arguments:
- hidden_states: bfloat16 [6144, 4096], P('sp'), may hold values from -60 to 60
- w_conv_b: bfloat16 [4096, 2048], P(None, 'tp'), may hold values from -0.09375 to 0.09375
- w_conv_c: bfloat16 [4096, 2048], P(None, 'tp'), may hold values from -0.09375 to 0.09375
- w_conv_h: bfloat16 [4096, 2048], P(None, 'tp'), may hold values from -0.09375 to 0.09375
- conv_taps: bfloat16 [3, 2048], P(None, 'tp'), may hold values from -3.5 to 3.5
- w_query: bfloat16 [4096, 2048], P(None, 'tp'), may hold values from -0.15625 to 0.15625
- w_key: bfloat16 [4096, 2048], P(None, 'tp'), may hold values from -0.09375 to 0.09375
- w_value: bfloat16 [4096, 2048], P(None, 'tp'), may hold values from -0.09375 to 0.09375
- lambdas: float32 [16], P('tp'), may hold values from 0.3 to 0.8
- head_gain: bfloat16 [128], replicated, may hold values from 0.099609375 to 1.8984375
- w_out_conv: bfloat16 [2048, 4096], P('tp'), may hold values from -1 to 1
- w_out_attn: bfloat16 [2048, 4096], P('tp'), may hold values from -1 to 1
- out_gain: bfloat16 [4096], replicated, may hold values from 0.099609375 to 1.8984375
Outputs:
- mixed: bfloat16 [6144, 4096], P('sp', 'tp')
The draws below stay inside these ranges and needn't reach their ends.
All inputs are finite; a program needn't handle non-finite values.
Results may differ from the reference program's by a relative error of at most 0.023.
Values may be sent and summed in bfloat16 or wider, within the bound.
A program may use at most 192 MiB of HBM per device.

```python
import jax
import jax.numpy as jnp
from jax import lax

D = 4096
HEADS = 16
QK = 64
CONV = 2048
TAPS = 3
TOK_DEV = 768
VD = 128
TOKENS = 6144
N_TP = 4


def draw_hidden_states(key, part):
    values = jnp.clip(jax.random.normal(key, (TOKENS, D), jnp.float32), -6.0, 6.0)
    return jnp.clip(values, -60.0, 60.0).astype(jnp.bfloat16)


def rising_columns(key, row_count):
    columns = jnp.arange(D, dtype=jnp.float32) / D
    base = jnp.clip(jax.random.normal(key, (row_count, D), jnp.float32), -6.0, 6.0)
    ramp = 3.0 ** columns
    values = base * ramp[None, :] * (CONV + HEADS * VD) ** (-0.5)
    return jnp.clip(values, -1.0, 1.0).astype(jnp.bfloat16)


def draw_w_out_conv(key, part):
    return rising_columns(jax.random.fold_in(key, 11), CONV)


def draw_w_out_attn(key, part):
    return rising_columns(jax.random.fold_in(key, 13), HEADS * VD)


def block_scale(own_key, shape, cuts, smallest, high):
    gain = 1.0
    for position, shards_of in cuts:
        draws = jax.random.uniform(jax.random.fold_in(jax.random.fold_in(own_key, 6), position), (shards_of,), jnp.float32, smallest / len(cuts), high / len(cuts))
        gain = gain * jnp.repeat(jnp.exp(draws), shape[position] // shards_of).reshape((-1,) + (1,) * (len(shape) - 1 - position))
    return gain


def normal_values(key, shape, width, most, cuts=(), kind=jnp.bfloat16):
    values = width * jax.random.normal(key, shape, jnp.float32)
    if cuts:
        values = values * block_scale(key, shape, cuts, -0.22, 0.18)
    return jnp.clip(values, -most, most).astype(kind)


def setup_inputs(seed: int = 0) -> dict:
    splits = jax.random.split(jax.random.key(seed), 14)
    return {
        "hidden_states": draw_hidden_states(jax.random.fold_in(splits[13], 71), 0),
        "w_conv_b": normal_values(splits[1], (D, CONV), D ** -0.5, 0.09375, ((1, 4),)),
        "w_conv_c": normal_values(splits[2], (D, CONV), D ** -0.5, 0.09375, ((1, 4),)),
        "w_conv_h": normal_values(splits[3], (D, CONV), D ** -0.5, 0.09375, ((1, 4),)),
        "conv_taps": normal_values(splits[4], (TAPS, CONV), TAPS ** -0.5, 3.5, ((1, 4),)),
        "w_query": normal_values(splits[5], (D, HEADS * 2 * QK), (D // 3) ** -0.5, 0.15625, ((1, 4),)),
        "w_key": normal_values(splits[6], (D, HEADS * 2 * QK), D ** -0.5, 0.09375, ((1, 4),)),
        "w_value": normal_values(splits[7], (D, HEADS * VD), D ** -0.5, 0.09375, ((1, 4),)),
        "lambdas": jnp.clip(0.3 + 0.5 * jax.random.uniform(splits[8], (HEADS,), jnp.float32) ** block_scale(splits[8], (HEADS,), ((0, 4),), -0.2, 0.2), 0.3, 0.8),
        "head_gain": jnp.clip(1.0 + 0.18 * jax.random.normal(splits[9], (VD,), jnp.float32), 0.099609375, 1.8984375).astype(jnp.bfloat16),
        "w_out_conv": draw_w_out_conv(jax.random.fold_in(splits[13], 71), 0),
        "w_out_attn": draw_w_out_attn(jax.random.fold_in(splits[13], 71), 0),
        "out_gain": jnp.clip(1.0 + 0.18 * jax.random.normal(splits[12], (D,), jnp.float32), 0.099609375, 1.8984375).astype(jnp.bfloat16),
    }


def rotate(values, positions):
    inverse = 1.0 / 10000.0 ** (jnp.arange(0, QK, 2, dtype=jnp.float32) / QK)
    angles = positions[:, None] * inverse[None, :]
    angles = jnp.concatenate([angles, angles], axis=-1)
    cosine = jnp.cos(angles)[:, None, None, :]
    sine = jnp.sin(angles)[:, None, None, :]
    first_half, second_half = jnp.split(values, 2, axis=-1)
    return values * cosine + jnp.concatenate([-second_half, first_half], axis=-1) * sine

def reference(hidden_states, w_conv_b, w_conv_c, w_conv_h, conv_taps, w_query, w_key, w_value, lambdas, head_gain, w_out_conv, w_out_attn, out_gain):

    def project(weight):
        return jnp.dot(hidden_states, weight, preferred_element_type=jnp.float32).astype(jnp.bfloat16)
    u_b = project(w_conv_b)
    u_c = project(w_conv_c)
    u_h = project(w_conv_h)
    gated = u_c.astype(jnp.float32) * u_h.astype(jnp.float32)
    padded = jnp.concatenate([jnp.zeros((TAPS - 1, CONV), jnp.float32), gated], axis=0)
    taps_f = conv_taps.astype(jnp.float32)
    convolved = jnp.zeros((TOKENS, CONV), jnp.float32)
    for tap in range(TAPS):
        convolved = convolved + taps_f[tap][None, :] * padded[tap:tap + TOKENS]
    conv_out = (u_b.astype(jnp.float32) * convolved).astype(jnp.bfloat16)
    positions = jnp.arange(TOKENS, dtype=jnp.float32)
    query = rotate(project(w_query).reshape(TOKENS, HEADS, 2, QK).astype(jnp.float32), positions).astype(jnp.bfloat16)
    keys = rotate(project(w_key).reshape(TOKENS, HEADS, 2, QK).astype(jnp.float32), positions).astype(jnp.bfloat16)
    values = project(w_value).reshape(TOKENS, HEADS, VD)
    gain_f = head_gain.astype(jnp.float32)
    key_pos = jnp.arange(TOKENS, dtype=jnp.int32)

    def one_head(args):
        head_query, head_keys, head_values, weight_two = args
        keys_f = head_keys.astype(jnp.float32)
        values_f = head_values.astype(jnp.float32)

        def one_block(block_index):
            first = (block_index * TOK_DEV).astype(jnp.int32)
            block_query = lax.dynamic_slice_in_dim(head_query, first, TOK_DEV, 0).astype(jnp.float32)
            scores = jnp.einsum('qcd,kcd->cqk', block_query, keys_f) * QK ** (-0.5)
            query_pos = first + jnp.arange(TOK_DEV, dtype=jnp.int32)
            visible = key_pos[None, :] <= query_pos[:, None]
            scores = jnp.where(visible[None], scores, -jnp.inf)
            top = lax.optimization_barrier(jnp.max(scores, axis=-1, keepdims=True))
            weights = jnp.exp(scores - top)
            denom = lax.optimization_barrier(jnp.sum(weights, axis=-1))
            rounded = lax.optimization_barrier(weights.astype(jnp.bfloat16)).astype(jnp.float32)
            numer = jnp.einsum('cqk,ke->cqe', rounded, values_f)
            diff = numer[0] / denom[0][:, None] - weight_two * numer[1] / denom[1][:, None]
            normed = diff * lax.rsqrt(lax.optimization_barrier(jnp.mean(diff * diff, axis=-1, keepdims=True)) + 1e-05) * gain_f[None, :]
            return normed.astype(jnp.bfloat16)
        blocks = lax.map(one_block, jnp.arange(TOKENS // TOK_DEV, dtype=jnp.int32))
        return blocks.reshape(TOKENS, VD)
    per_head = lax.map(one_head, (query.transpose(1, 0, 2, 3), keys.transpose(1, 0, 2, 3), values.transpose(1, 0, 2), lambdas))
    attn_out = per_head.transpose(1, 0, 2).reshape(TOKENS, HEADS * VD)
    conv_width = CONV // N_TP
    attn_width = HEADS * VD // N_TP
    total = jnp.zeros((TOKENS, D), jnp.float32)
    for block in range(N_TP):
        term = jnp.dot(conv_out[:, block * conv_width:(block + 1) * conv_width], w_out_conv[block * conv_width:(block + 1) * conv_width], preferred_element_type=jnp.float32)
        term = term + jnp.dot(attn_out[:, block * attn_width:(block + 1) * attn_width], w_out_attn[block * attn_width:(block + 1) * attn_width], preferred_element_type=jnp.float32)
        total = total + lax.optimization_barrier(term.astype(jnp.bfloat16)).astype(jnp.float32)
    mix = total.astype(jnp.bfloat16).astype(jnp.float32)
    mean_value = lax.optimization_barrier(jnp.mean(mix, axis=-1, keepdims=True))
    variance = lax.optimization_barrier(jnp.mean(mix * mix, axis=-1, keepdims=True)) - mean_value * mean_value
    normed = (mix - mean_value) * lax.rsqrt(variance + 1e-05) * out_gain.astype(jnp.float32)[None, :]
    return normed.astype(jnp.bfloat16)
```

```python
import functools
import math

import jax
import jax.numpy as jnp
from jax import lax
from jax.experimental import pallas as pl
from jax.experimental.pallas import tpu as pltpu
from jax.sharding import PartitionSpec as P

QK = 64
VD = 128
TILE = 256
NEG_LARGE = -1e30
VMEM_LIMIT = 60 * 1024 * 1024


def qkv_kernel(x_ref, wq_ref, wk_ref, wv_ref, cos_ref, sin_ref, q_ref, kv_ref):
    x = x_ref[...]
    lane = lax.broadcasted_iota(jnp.int32, cos_ref.shape, 1)
    low = lane % QK < QK // 2

    def project(w_ref):
        return jnp.dot(x, w_ref[...], preferred_element_type=jnp.float32).astype(jnp.bfloat16)

    def rotate(values):
        values = values.astype(jnp.float32)
        partner = jnp.where(
            low, pltpu.roll(values, VD - QK // 2, 1), pltpu.roll(values, QK // 2, 1)
        )
        return values * cos_ref[...] + partner * sin_ref[...]

    fold = QK ** (-0.5) * math.log2(math.e)
    q, k, v = project(wq_ref), project(wk_ref), project(wv_ref)
    for h in range(TILE // VD):
        cols = slice(h * VD, (h + 1) * VD)
        q_ref[h] = (rotate(q[:, cols]) * fold).astype(jnp.bfloat16)
        kv_ref[0, h] = rotate(k[:, cols]).astype(jnp.bfloat16)
        kv_ref[1, h] = v[:, cols]


def conv_kernel(x_ref, rim_ref, wb_ref, wc_ref, wh_ref, taps_ref, out_ref):
    x, rim = x_ref[...], rim_ref[...]

    def project(rows, w_ref):
        return (
            jnp.dot(rows, w_ref[...], preferred_element_type=jnp.float32)
            .astype(jnp.bfloat16)
            .astype(jnp.float32)
        )

    gated = project(x, wc_ref) * project(x, wh_ref)
    before = project(rim, wc_ref) * project(rim, wh_ref)
    last = rim.shape[0]
    one, two = before[last - 1 :], before[last - 2 : last - 1]
    row = lax.broadcasted_iota(jnp.int32, gated.shape, 0)
    back_one = jnp.where(row == 0, one, pltpu.roll(gated, 1, 0))
    back_two = jnp.where(row == 0, two, jnp.where(row == 1, one, pltpu.roll(gated, 2, 0)))
    taps = taps_ref[...].astype(jnp.float32)
    conv = taps[0:1] * back_two + taps[1:2] * back_one + taps[2:3] * gated
    out_ref[...] = (project(x, wb_ref) * conv).astype(jnp.bfloat16)


def attention_kernel(
    parts, meta, q_ref, k_ref, v_ref, lam_ref, gain_ref, o_ref, m_ref, l_ref, acc_ref
):
    i = pl.program_id(0)
    blocks, block, _ = k_ref.shape
    rows = q_ref.shape[1]
    q = q_ref[0]
    lane = lax.broadcasted_iota(jnp.int32, q.shape, 1)
    zero = jnp.zeros_like(q)
    maps = (jnp.where(lane < QK, q, zero), jnp.where(lane < QK, zero, q))
    m_ref[...] = jnp.full(m_ref.shape, NEG_LARGE, jnp.float32)
    l_ref[...] = jnp.zeros(l_ref.shape, jnp.float32)
    acc_ref[...] = jnp.zeros(acc_ref.shape, jnp.float32)
    part = meta[3 * blocks]
    part = jnp.where(i % 2 == 0, part, parts - 1 - part)

    def visit(kb, masked):
        k, v = k_ref[meta[blocks + kb]], v_ref[meta[2 * blocks + kb]]
        for c in range(2):
            s = lax.dot_general(
                maps[c], k, (((1,), (1,)), ((), ())), preferred_element_type=jnp.float32
            )
            if masked:
                r = part * rows + lax.broadcasted_iota(jnp.int32, s.shape, 0)
                s = jnp.where(lax.broadcasted_iota(jnp.int32, s.shape, 1) <= r, s, NEG_LARGE)
            old = m_ref[c]
            new = jnp.maximum(old, jnp.max(s, axis=1, keepdims=True))
            factor = jnp.exp2(old - new)
            total = l_ref[c] * factor
            pieces = []
            for b in range(block // 128):
                w = jnp.exp2(s[:, b * 128 : (b + 1) * 128] - new)
                total = total + w
                pieces.append(w.astype(jnp.bfloat16))
            m_ref[c] = new
            l_ref[c] = total
            acc_ref[c] = acc_ref[c] * factor + jnp.dot(
                jnp.concatenate(pieces, axis=1), v, preferred_element_type=jnp.float32
            )

    @pl.loop(0, i)
    def _(kb):
        visit(kb, False)

    visit(i, True)
    diff = acc_ref[0] / jnp.sum(l_ref[0], axis=1, keepdims=True) - lam_ref[0] * acc_ref[1] / jnp.sum(
        l_ref[1], axis=1, keepdims=True
    )
    norm = lax.rsqrt(jnp.mean(diff * diff, axis=1, keepdims=True) + 1e-05)
    o_ref[0] = (diff * norm * gain_ref[...].astype(jnp.float32)).astype(jnp.bfloat16)


def per_device(
    n,
    tp,
    hidden_states,
    w_conv_b,
    w_conv_c,
    w_conv_h,
    conv_taps,
    w_query,
    w_key,
    w_value,
    lambdas,
    head_gain,
    w_out_conv,
    w_out_attn,
    out_gain,
):
    tok, model = hidden_states.shape
    heads = w_value.shape[1] // VD
    channels = w_conv_b.shape[1]
    j, t = lax.axis_index("sp"), lax.axis_index("tp")
    c, y = t % 2, t // 2
    half = n // 2
    repeat = half // heads
    parts = 2 * repeat
    rows = tok // parts
    pair = [(a, a ^ 1) for a in range(tp)]

    rim = lax.ppermute(hidden_states[tok - 16 :], "sp", [(a, a + 1) for a in range(n - 1)])
    other_lambdas = lax.ppermute(lambdas, "tp", pair)

    inverse = 1.0 / 10000.0 ** (jnp.arange(0, QK, 2, dtype=jnp.float32) / QK)
    positions = (j * tok + jnp.arange(tok, dtype=jnp.int32)).astype(jnp.float32)
    angles = positions[:, None] * inverse[None, :]
    cos, sin = jnp.cos(angles), jnp.sin(angles)
    cos = jnp.concatenate([cos] * 4, axis=1)
    sin = jnp.concatenate([-sin, sin] * 2, axis=1)

    whole = lambda *shape: pl.BlockSpec(shape, lambda i: (0,) * len(shape))
    tile = lambda depth: pl.BlockSpec((depth, TILE), lambda i: (0, i))
    per = TILE // VD
    flops = 6 * tok * model * channels
    query, keyval = pl.pallas_call(
        qkv_kernel,
        grid=(heads * VD // TILE,),
        out_shape=(
            jax.ShapeDtypeStruct((heads, tok, VD), jnp.bfloat16),
            jax.ShapeDtypeStruct((2, heads, tok, VD), jnp.bfloat16),
        ),
        in_specs=[whole(tok, model)] + [tile(model)] * 3 + [whole(tok, VD)] * 2,
        out_specs=(
            pl.BlockSpec((per, tok, VD), lambda i: (i, 0, 0)),
            pl.BlockSpec((2, per, tok, VD), lambda i: (0, i, 0, 0)),
        ),
        compiler_params=pltpu.CompilerParams(vmem_limit_bytes=VMEM_LIMIT),
        cost_estimate=pl.CostEstimate(
            flops=flops, bytes_accessed=2 * model * (tok + 3 * channels), transcendentals=0
        ),
        name="qkv",
    )(hidden_states, w_query, w_key, w_value, cos, sin)

    steps = [(k, e) for k in range(half) for e in range(2)]

    def route(k, e):
        pairs = []
        for a in range(n):
            for b in range(tp):
                s = (b % 2) * half + (a + k) % half
                core = (a // half + e) % 2
                pairs.append((a * tp + b, s * tp + b // 2 * 2 + core))
        return pairs

    def sent(k, e):
        s = (j + k) % half
        head, rep, core = s // repeat, s % repeat, (j // half + e) % 2
        part = rep * 2 + core
        return head, jnp.where(j % 2 == 0, part, parts - 1 - part), core

    messages = []
    for k, e in steps:
        head, part, core = sent(k, e)
        q_rows = lax.dynamic_slice(query, (head, part * rows, 0), (1, rows, VD))
        kv_rows = lax.dynamic_slice(keyval, (core, head, 0, 0), (1, 1, tok, VD))
        message = jnp.concatenate([q_rows[0], kv_rows[0, 0]], axis=0)
        messages.append(lax.ppermute(message, ("sp", "tp"), route(k, e)))

    conv_out = pl.pallas_call(
        conv_kernel,
        grid=(channels // TILE,),
        out_shape=jax.ShapeDtypeStruct((tok, channels), jnp.bfloat16),
        in_specs=[whole(tok, model), whole(16, model)]
        + [tile(model)] * 3
        + [tile(conv_taps.shape[0])],
        out_specs=tile(tok),
        compiler_params=pltpu.CompilerParams(vmem_limit_bytes=VMEM_LIMIT),
        cost_estimate=pl.CostEstimate(
            flops=flops, bytes_accessed=2 * model * (tok + 3 * channels), transcendentals=0
        ),
        name="conv",
    )(hidden_states, rim, w_conv_b, w_conv_c, w_conv_h, conv_taps)

    conv_out, *messages = lax.optimization_barrier((conv_out, *messages))
    arrived = jnp.stack(messages)
    mine = arrived[:, rows:]
    other = lax.ppermute(mine, "tp", pair)
    keys = jnp.where(c == 0, mine, other)
    values = jnp.where(c == 0, other, mine)
    source = jnp.arange(n, dtype=jnp.int32)
    slots = [2 * ((j - source) % half) + (core - source // half) % 2 for core in (c, 0, 1)]
    meta = jnp.concatenate(slots + [((j % repeat) * 2 + c)[None]]).astype(jnp.int32)
    chip_lambdas = jnp.where(
        c == 0,
        jnp.concatenate([lambdas, other_lambdas]),
        jnp.concatenate([other_lambdas, lambdas]),
    )
    lam = lax.dynamic_slice(chip_lambdas, (j // repeat,), (1,))

    fixed = lambda *shape: pl.BlockSpec(shape, lambda i, m: (0,) * len(shape))
    slotted = pl.BlockSpec((1, rows, VD), lambda i, m: (m[i], 0, 0))
    attended = pl.pallas_call(
        functools.partial(attention_kernel, parts),
        grid_spec=pltpu.PrefetchScalarGridSpec(
            num_scalar_prefetch=1,
            grid=(n,),
            in_specs=[
                slotted,
                fixed(n, tok, VD),
                fixed(n, tok, VD),
                pl.BlockSpec(memory_space=pltpu.SMEM),
                fixed(1, VD),
            ],
            out_specs=slotted,
            scratch_shapes=[pltpu.VMEM((2, rows, VD), jnp.float32)] * 3,
        ),
        out_shape=jax.ShapeDtypeStruct((n, rows, VD), jnp.bfloat16),
        compiler_params=pltpu.CompilerParams(vmem_limit_bytes=VMEM_LIMIT),
        cost_estimate=pl.CostEstimate(
            flops=4 * n * n * rows * tok * VD, bytes_accessed=4 * n * tok * VD, transcendentals=0
        ),
        name="attention",
    )(meta, arrived, keys, values, lam, head_gain[None])

    attn_out = jnp.zeros((tok, heads * VD), jnp.bfloat16)
    for index, (k, e) in enumerate(steps):
        back = [(b, a) for a, b in route(k, e)]
        piece = lax.ppermute(attended[index], ("sp", "tp"), back)
        head, part, _ = sent(k, e)
        attn_out = lax.dynamic_update_slice(attn_out, piece, (part * rows, head * VD))

    ranks = tp // 2
    width = model // tp

    def partial_sum(rank):
        cols = lambda w: lax.dynamic_slice_in_dim(w, rank * 2 * width, 2 * width, 1)
        value = jnp.dot(
            conv_out, cols(w_out_conv), preferred_element_type=jnp.float32
        ) + jnp.dot(attn_out, cols(w_out_attn), preferred_element_type=jnp.float32)
        value = value.astype(jnp.bfloat16)
        own = jnp.where(c == 0, value[:, :width], value[:, width:])
        away = jnp.where(c == 0, value[:, width:], value[:, :width])
        return own.astype(jnp.float32) + lax.ppermute(away, "tp", pair).astype(jnp.float32)

    arriving = []
    for step in range(1, ranks):
        total = partial_sum((y + step) % ranks).astype(jnp.bfloat16)
        onward = [(a, (a // 2 + step) % ranks * 2 + a % 2) for a in range(tp)]
        arriving.append(lax.ppermute(total, "tp", onward))
    mix = partial_sum(y)
    for block in arriving:
        mix = mix + block.astype(jnp.float32)
    mix_f = mix.astype(jnp.bfloat16).astype(jnp.float32)
    total_sum, total_squares = lax.psum(
        (jnp.sum(mix_f, axis=-1), jnp.sum(mix_f * mix_f, axis=-1)), "tp"
    )
    mean_value = (total_sum / model)[:, None]
    variance = (total_squares / model)[:, None] - mean_value * mean_value
    own_gain = lax.dynamic_slice_in_dim(out_gain, t * width, width, 0).astype(jnp.float32)
    return ((mix_f - mean_value) * lax.rsqrt(variance + 1e-05) * own_gain[None, :]).astype(
        jnp.bfloat16
    )


def solution(mesh):
    n, tp = mesh.shape["sp"], mesh.shape["tp"]
    return jax.shard_map(
        functools.partial(per_device, n, tp),
        mesh=mesh,
        in_specs=(
            P("sp", None),
            P(None, "tp"),
            P(None, "tp"),
            P(None, "tp"),
            P(None, "tp"),
            P(None, "tp"),
            P(None, "tp"),
            P(None, "tp"),
            P("tp"),
            P(),
            P("tp", None),
            P("tp", None),
            P(),
        ),
        out_specs=P("sp", "tp"),
        check_vma=False,
    )
```

```python
import functools
import math

import jax
import jax.numpy as jnp
from jax import lax
from jax.experimental import pallas as pl
from jax.experimental.pallas import tpu as pltpu
from jax.sharding import PartitionSpec as P

QK = 64
VD = 128
TILE = 256
NEG_LARGE = -1e30
VMEM_LIMIT = 60 * 1024 * 1024


def qkv_kernel(x_ref, wq_ref, wk_ref, wv_ref, cos_ref, sin_ref, q_ref, kv_ref):
    x = x_ref[...]
    lane = lax.broadcasted_iota(jnp.int32, cos_ref.shape, 1)
    low = lane % QK < QK // 2

    def project(w_ref):
        return jnp.dot(x, w_ref[...], preferred_element_type=jnp.float32).astype(jnp.bfloat16)

    def rotate(values):
        values = values.astype(jnp.float32)
        partner = jnp.where(
            low, pltpu.roll(values, VD - QK // 2, 1), pltpu.roll(values, QK // 2, 1)
        )
        return values * cos_ref[...] + partner * sin_ref[...]

    fold = QK ** (-0.5) * math.log2(math.e)
    q, k, v = project(wq_ref), project(wk_ref), project(wv_ref)
    for h in range(TILE // VD):
        cols = slice(h * VD, (h + 1) * VD)
        q_ref[h] = (rotate(q[:, cols]) * fold).astype(jnp.bfloat16)
        kv_ref[0, h] = rotate(k[:, cols]).astype(jnp.bfloat16)
        kv_ref[1, h] = v[:, cols]


def conv_kernel(x_ref, rim_ref, wb_ref, wc_ref, wh_ref, taps_ref, out_ref):
    x, rim = x_ref[...], rim_ref[...]

    def project(rows, w_ref):
        return (
            jnp.dot(rows, w_ref[...], preferred_element_type=jnp.float32)
            .astype(jnp.bfloat16)
            .astype(jnp.float32)
        )

    gated = project(x, wc_ref) * project(x, wh_ref)
    before = project(rim, wc_ref) * project(rim, wh_ref)
    last = rim.shape[0]
    one, two = before[last - 1 :], before[last - 2 : last - 1]
    row = lax.broadcasted_iota(jnp.int32, gated.shape, 0)
    back_one = jnp.where(row == 0, one, pltpu.roll(gated, 1, 0))
    back_two = jnp.where(row == 0, two, jnp.where(row == 1, one, pltpu.roll(gated, 2, 0)))
    taps = taps_ref[...].astype(jnp.float32)
    conv = taps[0:1] * back_two + taps[1:2] * back_one + taps[2:3] * gated
    out_ref[...] = (project(x, wb_ref) * conv).astype(jnp.bfloat16)


def attention_kernel(
    parts, meta, q_ref, k_ref, v_ref, lam_ref, gain_ref, o_ref, m_ref, l_ref, acc_ref
):
    i = pl.program_id(0)
    blocks, block, _ = k_ref.shape
    rows = q_ref.shape[1]
    q = q_ref[0]
    lane = lax.broadcasted_iota(jnp.int32, q.shape, 1)
    zero = jnp.zeros_like(q)
    both = jnp.concatenate(
        [jnp.where(lane < QK, q, zero), jnp.where(lane < QK, zero, q)], axis=0
    )
    m_ref[...] = jnp.full(m_ref.shape, NEG_LARGE, jnp.float32)
    l_ref[...] = jnp.zeros(l_ref.shape, jnp.float32)
    acc_ref[...] = jnp.zeros(acc_ref.shape, jnp.float32)
    part = meta[3 * blocks]
    part = jnp.where(i % 2 == 0, part, parts - 1 - part)

    def visit(kb, masked):
        k, v = k_ref[meta[blocks + kb]], v_ref[meta[2 * blocks + kb]]
        s = lax.dot_general(both, k, (((1,), (1,)), ((), ())), preferred_element_type=jnp.float32)
        if masked:
            r = part * rows + lax.broadcasted_iota(jnp.int32, s.shape, 0) % rows
            s = jnp.where(lax.broadcasted_iota(jnp.int32, s.shape, 1) <= r, s, NEG_LARGE)
        slabs = [s[:, b * VD : (b + 1) * VD] for b in range(block // VD)]
        old = m_ref[...]
        top = functools.reduce(jnp.maximum, slabs)
        new = jnp.maximum(old, jnp.max(top, axis=1, keepdims=True))
        factor = jnp.exp2(old - new)
        total = l_ref[...] * factor
        weights = []
        for slab in slabs:
            w = jnp.exp2(slab - new)
            total = total + w
            weights.append(w.astype(jnp.bfloat16))
        m_ref[...] = new
        l_ref[...] = total
        acc_ref[...] = acc_ref[...] * factor + jnp.dot(
            jnp.concatenate(weights, axis=1), v, preferred_element_type=jnp.float32
        )

    @pl.loop(0, i)
    def _(kb):
        visit(kb, False)

    visit(i, True)
    first, second = (
        acc_ref[half] / jnp.sum(l_ref[half], axis=1, keepdims=True)
        for half in (pl.ds(0, rows), pl.ds(rows, rows))
    )
    diff = first - lam_ref[0] * second
    norm = lax.rsqrt(jnp.mean(diff * diff, axis=1, keepdims=True) + 1e-05)
    o_ref[0] = (diff * norm * gain_ref[...].astype(jnp.float32)).astype(jnp.bfloat16)


def per_device(
    n,
    tp,
    hidden_states,
    w_conv_b,
    w_conv_c,
    w_conv_h,
    conv_taps,
    w_query,
    w_key,
    w_value,
    lambdas,
    head_gain,
    w_out_conv,
    w_out_attn,
    out_gain,
):
    tok, model = hidden_states.shape
    heads = w_value.shape[1] // VD
    channels = w_conv_b.shape[1]
    j, t = lax.axis_index("sp"), lax.axis_index("tp")
    c, y = t % 2, t // 2
    half = n // 2
    repeat = half // heads
    parts = 2 * repeat
    rows = tok // parts
    pair = [(a, a ^ 1) for a in range(tp)]

    rim = lax.ppermute(hidden_states[tok - 16 :], "sp", [(a, a + 1) for a in range(n - 1)])
    other_lambdas = lax.ppermute(lambdas, "tp", pair)

    inverse = 1.0 / 10000.0 ** (jnp.arange(0, QK, 2, dtype=jnp.float32) / QK)
    positions = (j * tok + jnp.arange(tok, dtype=jnp.int32)).astype(jnp.float32)
    angles = positions[:, None] * inverse[None, :]
    cos, sin = jnp.cos(angles), jnp.sin(angles)
    cos = jnp.concatenate([cos] * 4, axis=1)
    sin = jnp.concatenate([-sin, sin] * 2, axis=1)

    whole = lambda *shape: pl.BlockSpec(shape, lambda i: (0,) * len(shape))
    tile = lambda depth: pl.BlockSpec((depth, TILE), lambda i: (0, i))
    per = TILE // VD
    flops = 6 * tok * model * channels
    query, keyval = pl.pallas_call(
        qkv_kernel,
        grid=(heads * VD // TILE,),
        out_shape=(
            jax.ShapeDtypeStruct((heads, tok, VD), jnp.bfloat16),
            jax.ShapeDtypeStruct((2, heads, tok, VD), jnp.bfloat16),
        ),
        in_specs=[whole(tok, model)] + [tile(model)] * 3 + [whole(tok, VD)] * 2,
        out_specs=(
            pl.BlockSpec((per, tok, VD), lambda i: (i, 0, 0)),
            pl.BlockSpec((2, per, tok, VD), lambda i: (0, i, 0, 0)),
        ),
        compiler_params=pltpu.CompilerParams(vmem_limit_bytes=VMEM_LIMIT),
        cost_estimate=pl.CostEstimate(
            flops=flops, bytes_accessed=2 * model * (tok + 3 * channels), transcendentals=0
        ),
        name="qkv",
    )(hidden_states, w_query, w_key, w_value, cos, sin)

    steps = [(k, e) for k in range(half) for e in range(2)]

    def route(k, e):
        pairs = []
        for a in range(n):
            for b in range(tp):
                s = (b % 2) * half + (a + k) % half
                core = (a // half + e) % 2
                pairs.append((a * tp + b, s * tp + b // 2 * 2 + core))
        return pairs

    def sent(k, e):
        s = (j + k) % half
        head, rep, core = s // repeat, s % repeat, (j // half + e) % 2
        part = rep * 2 + core
        return head, jnp.where(j % 2 == 0, part, parts - 1 - part), core

    messages = []
    for k, e in steps:
        head, part, core = sent(k, e)
        q_rows = lax.dynamic_slice(query, (head, part * rows, 0), (1, rows, VD))
        kv_rows = lax.dynamic_slice(keyval, (core, head, 0, 0), (1, 1, tok, VD))
        message = jnp.concatenate([q_rows[0], kv_rows[0, 0]], axis=0)
        messages.append(lax.ppermute(message, ("sp", "tp"), route(k, e)))

    conv_out = pl.pallas_call(
        conv_kernel,
        grid=(channels // TILE,),
        out_shape=jax.ShapeDtypeStruct((tok, channels), jnp.bfloat16),
        in_specs=[whole(tok, model), whole(16, model)]
        + [tile(model)] * 3
        + [tile(conv_taps.shape[0])],
        out_specs=tile(tok),
        compiler_params=pltpu.CompilerParams(vmem_limit_bytes=VMEM_LIMIT),
        cost_estimate=pl.CostEstimate(
            flops=flops, bytes_accessed=2 * model * (tok + 3 * channels), transcendentals=0
        ),
        name="conv",
    )(hidden_states, rim, w_conv_b, w_conv_c, w_conv_h, conv_taps)

    conv_out, *messages = lax.optimization_barrier((conv_out, *messages))
    arrived = jnp.stack(messages)
    mine = arrived[:, rows:]
    other = lax.ppermute(mine, "tp", pair)
    keys = jnp.where(c == 0, mine, other)
    values = jnp.where(c == 0, other, mine)
    source = jnp.arange(n, dtype=jnp.int32)
    slots = [2 * ((j - source) % half) + (core - source // half) % 2 for core in (c, 0, 1)]
    meta = jnp.concatenate(slots + [((j % repeat) * 2 + c)[None]]).astype(jnp.int32)
    chip_lambdas = jnp.where(
        c == 0,
        jnp.concatenate([lambdas, other_lambdas]),
        jnp.concatenate([other_lambdas, lambdas]),
    )
    lam = lax.dynamic_slice(chip_lambdas, (j // repeat,), (1,))

    fixed = lambda *shape: pl.BlockSpec(shape, lambda i, m: (0,) * len(shape))
    slotted = pl.BlockSpec((1, rows, VD), lambda i, m: (m[i], 0, 0))
    attended = pl.pallas_call(
        functools.partial(attention_kernel, parts),
        grid_spec=pltpu.PrefetchScalarGridSpec(
            num_scalar_prefetch=1,
            grid=(n,),
            in_specs=[
                slotted,
                fixed(n, tok, VD),
                fixed(n, tok, VD),
                pl.BlockSpec(memory_space=pltpu.SMEM),
                fixed(1, VD),
            ],
            out_specs=slotted,
            scratch_shapes=[pltpu.VMEM((2 * rows, VD), jnp.float32)] * 3,
        ),
        out_shape=jax.ShapeDtypeStruct((n, rows, VD), jnp.bfloat16),
        compiler_params=pltpu.CompilerParams(vmem_limit_bytes=VMEM_LIMIT),
        cost_estimate=pl.CostEstimate(
            flops=4 * n * n * rows * tok * VD, bytes_accessed=4 * n * tok * VD, transcendentals=0
        ),
        name="attention",
    )(meta, arrived, keys, values, lam, head_gain[None])

    attn_out = jnp.zeros((tok, heads * VD), jnp.bfloat16)
    for index, (k, e) in enumerate(steps):
        back = [(b, a) for a, b in route(k, e)]
        piece = lax.ppermute(attended[index], ("sp", "tp"), back)
        head, part, _ = sent(k, e)
        attn_out = lax.dynamic_update_slice(attn_out, piece, (part * rows, head * VD))

    ranks = tp // 2
    width = model // tp

    def halves(rank, conv_rows, attn_rows):
        cols = lambda w: lax.dynamic_slice_in_dim(w, rank * 2 * width, 2 * width, 1)
        value = jnp.dot(
            conv_rows, cols(w_out_conv), preferred_element_type=jnp.float32
        ) + jnp.dot(attn_rows, cols(w_out_attn), preferred_element_type=jnp.float32)
        value = value.astype(jnp.bfloat16)
        own = jnp.where(c == 0, value[:, :width], value[:, width:])
        away = jnp.where(c == 0, value[:, width:], value[:, :width])
        return own, away

    def pair_sum(own, away):
        return own.astype(jnp.float32) + lax.ppermute(away, "tp", pair).astype(jnp.float32)

    arriving, totals = [], []
    chunk = tok // 2
    for step in range(1, ranks):
        onward = [(a, (a // 2 + step) % ranks * 2 + a % 2) for a in range(tp)]
        blocks = []
        for first in (0, chunk):
            rows_of = slice(first, first + chunk)
            own, away = halves((y + step) % ranks, conv_out[rows_of], attn_out[rows_of])
            total = pair_sum(own, away).astype(jnp.bfloat16)
            totals.append(total)
            blocks.append(lax.ppermute(total, "tp", onward))
        arriving.append(blocks)
    conv_late, attn_late, *_ = lax.optimization_barrier((conv_out, attn_out, *totals))
    own, away = halves(y, conv_late, attn_late)
    if arriving:
        own, away, arriving[0][0] = lax.optimization_barrier((own, away, arriving[0][0]))
    mix = pair_sum(own, away)
    for blocks in arriving:
        mix = mix + jnp.concatenate(blocks, axis=0).astype(jnp.float32)
    mix_f = mix.astype(jnp.bfloat16).astype(jnp.float32)
    total_sum, total_squares = lax.psum(
        (jnp.sum(mix_f, axis=-1), jnp.sum(mix_f * mix_f, axis=-1)), "tp"
    )
    mean_value = (total_sum / model)[:, None]
    variance = (total_squares / model)[:, None] - mean_value * mean_value
    own_gain = lax.dynamic_slice_in_dim(out_gain, t * width, width, 0).astype(jnp.float32)
    return ((mix_f - mean_value) * lax.rsqrt(variance + 1e-05) * own_gain[None, :]).astype(
        jnp.bfloat16
    )


def solution(mesh):
    n, tp = mesh.shape["sp"], mesh.shape["tp"]
    return jax.shard_map(
        functools.partial(per_device, n, tp),
        mesh=mesh,
        in_specs=(
            P("sp", None),
            P(None, "tp"),
            P(None, "tp"),
            P(None, "tp"),
            P(None, "tp"),
            P(None, "tp"),
            P(None, "tp"),
            P(None, "tp"),
            P("tp"),
            P(),
            P("tp", None),
            P("tp", None),
            P(),
        ),
        out_specs=P("sp", "tp"),
        check_vma=False,
    )
```
